32 devices in a mesh: fs: 4 (over z), rep: 4 (over y, x), tp: 2 (over core).
Axes of the slice: x: 2, y: 2, z: 4, core: 2. Of those that a mesh axis runs over, the one named last changes fastest.
Arguments:
- saved_in: bfloat16 [4096, 4096], P(('fs', 'rep', 'tp')), may hold values from -6 to 6
- out_cot: bfloat16 [4096, 4096], P(('fs', 'rep', 'tp')), may hold values from -0.09375 to 0.09375
- value_cot: bfloat16 [4096, 2048], P(('fs', 'rep'), 'tp'), may hold values from -0.09375 to 0.09375
- mixed_out: bfloat16 [4096, 2048], P(('fs', 'rep'), 'tp'), may hold values from -6 to 6
- value_factor: bfloat16 [4096, 512], P('fs'), may hold values from -0.09375 to 0.09375
- out_factor: bfloat16 [4096, 512], P('fs'), may hold values from -0.09375 to 0.09375
- value_weight: float32 [4096, 2048], P('fs', 'tp'), may hold values from -0.09375 to 0.09375
- out_weight: float32 [2048, 4096], P('tp', 'fs'), may hold values from -0.125 to 0.125
- value_first: float32 [512, 2048], P('fs', 'tp'), may hold values from -6 to 6
- value_second: float32 [512, 2048], P('fs', 'tp'), may hold values from 0.25 to 4
- out_first: float32 [512, 2048], P('fs', 'tp'), may hold values from -6 to 6
- out_second: float32 [512, 2048], P('fs', 'tp'), may hold values from 0.25 to 4
Outputs:
- value_weight_new: float32 [4096, 2048], P('fs', 'tp')
- value_weight_copy: bfloat16 [4096, 2048], P('fs', 'tp')
- out_weight_new: float32 [2048, 4096], P('tp', 'fs')
- out_weight_copy: bfloat16 [2048, 4096], P('tp', 'fs')
- value_first_new: float32 [512, 2048], P('fs', 'tp')
- value_second_new: float32 [512, 2048], P('fs', 'tp')
- out_first_new: float32 [512, 2048], P('fs', 'tp')
- out_second_new: float32 [512, 2048], P('fs', 'tp')
- value_step: float32 [512, 2048], P('fs', 'tp')
- out_step: float32 [512, 2048], P('fs', 'tp')
The draws below stay inside these ranges and needn't reach their ends.
All inputs are finite; a program needn't handle non-finite values.
Results may differ from the reference program's by a relative error of at most 0.005.
Values may be sent and summed in bfloat16 or wider, within the bound.
A program may use at most 128 MiB of HBM per device.

```python
import math
import jax
import jax.numpy as jnp

MODEL_DIM = 4096
CHANNELS = 2048
RANK = 512
TOKENS = 4096


def steps_of(stream_key, shape, pieces, least, largest):
    def one(position, blocks):
        draws = jax.random.uniform(jax.random.fold_in(jax.random.fold_in(stream_key, 6), position), (blocks,), jnp.float32, least / len(pieces), largest / len(pieces))
        return jnp.repeat(jnp.exp(draws), shape[position] // blocks).reshape((-1,) + (1,) * (len(shape) - position - 1))

    level = one(*pieces[0])
    for cut in pieces[1:]:
        level = level * one(*cut)
    return level


def bell_draw(rng, extent, scale, most, split=(), held_as=jnp.bfloat16):
    factor_of = steps_of(rng, extent, split, -0.22, 0.18) if split else 1.0
    drawn = jax.random.normal(rng, extent, jnp.float32) * scale * factor_of
    return jnp.minimum(jnp.maximum(drawn, -most), most).astype(held_as)


def setup_inputs(seed: int = 0) -> dict:
    arg_keys = jax.random.split(jax.random.key(seed), 13)
    return {
        "saved_in": bell_draw(arg_keys[0], (TOKENS, MODEL_DIM), 1.0, 6.0, ((0, 32),)),
        "out_cot": bell_draw(arg_keys[1], (TOKENS, MODEL_DIM), (TOKENS ** -0.5), 0.09375, ((0, 32),)),
        "value_cot": bell_draw(arg_keys[2], (TOKENS, CHANNELS), (TOKENS ** -0.5), 0.09375, ((0, 16), (1, 2))),
        "mixed_out": bell_draw(arg_keys[3], (TOKENS, CHANNELS), 1.0, 6.0, ((0, 16), (1, 2))),
        "value_factor": bell_draw(arg_keys[4], (MODEL_DIM, RANK), MODEL_DIM ** -0.5, 0.09375, ((0, 4),)),
        "out_factor": bell_draw(arg_keys[5], (MODEL_DIM, RANK), MODEL_DIM ** -0.5, 0.09375, ((0, 4),)),
        "value_weight": bell_draw(arg_keys[6], (MODEL_DIM, CHANNELS), MODEL_DIM ** -0.5, 0.09375, ((0, 4), (1, 2)), jnp.float32),
        "out_weight": bell_draw(arg_keys[7], (CHANNELS, MODEL_DIM), CHANNELS ** -0.5, 0.125, ((0, 2), (1, 4)), jnp.float32),
        "value_first": bell_draw(arg_keys[8], (RANK, CHANNELS), 1.0, 6.0, ((0, 4), (1, 2)), jnp.float32),
        "value_second": jnp.clip(jnp.exp(math.log(4.0) - 2.7725887 * jax.random.uniform(arg_keys[9], (RANK, CHANNELS), jnp.float32) ** steps_of(arg_keys[9], (RANK, CHANNELS), ((0, 4), (1, 2)), -0.2, 0.2)), 0.25, 4.0),
        "out_first": bell_draw(arg_keys[10], (RANK, CHANNELS), 1.0, 6.0, ((0, 4), (1, 2)), jnp.float32),
        "out_second": jnp.clip(jnp.exp(math.log(4.0) - 2.7725887 * jax.random.uniform(arg_keys[11], (RANK, CHANNELS), jnp.float32) ** steps_of(arg_keys[11], (RANK, CHANNELS), ((0, 4), (1, 2)), -0.2, 0.2)), 0.25, 4.0),
    }


beta_first = 0.8
beta_second = 0.9
step_rate = 0.05
clip_level = 0.5

def adapt(grad, first, second):
    new_first = beta_first * first + (1.0 - beta_first) * grad
    new_second = beta_second * second + (1.0 - beta_second) * grad * grad
    lowered = (new_first / jnp.sqrt(new_second)).astype(jnp.bfloat16)
    return (new_first, new_second, lowered)

def reference(saved_in, out_cot, value_cot, mixed_out, value_factor, out_factor, value_weight, out_weight, value_first, value_second, out_first, out_second):
    proj_in = jnp.dot(saved_in, value_factor, preferred_element_type=jnp.float32).astype(jnp.bfloat16)
    proj_cot = jnp.dot(out_cot, out_factor, preferred_element_type=jnp.float32).astype(jnp.bfloat16)
    grad_value = jnp.dot(proj_in.T, value_cot, preferred_element_type=jnp.float32)
    grad_out = jnp.dot(proj_cot.T, mixed_out, preferred_element_type=jnp.float32)
    value_first_new, value_second_new, low_value = adapt(grad_value, value_first, value_second)
    out_first_new, out_second_new, low_out = adapt(grad_out, out_first, out_second)
    value_float = low_value.astype(jnp.float32)
    out_float = low_out.astype(jnp.float32)
    total = jnp.sum(value_float * value_float) + jnp.sum(out_float * out_float)
    spread = jnp.sqrt(total / (2.0 * RANK * CHANNELS))
    scale = clip_level / jnp.maximum(spread, clip_level)
    value_full = jnp.dot(value_factor, low_value, preferred_element_type=jnp.float32)
    out_full = jnp.dot(low_out.T, out_factor.T, preferred_element_type=jnp.float32)
    value_weight_new = value_weight - step_rate * scale * value_full
    out_weight_new = out_weight - step_rate * scale * out_full
    return (value_weight_new, value_weight_new.astype(jnp.bfloat16), out_weight_new, out_weight_new.astype(jnp.bfloat16), value_first_new, value_second_new, out_first_new, out_second_new, scale * value_float, scale * out_float)
```

```python
import functools

import jax
import jax.numpy as jnp
from jax import lax
from jax.experimental import pallas as pl
from jax.experimental.pallas import tpu as pltpu
from jax.sharding import PartitionSpec as P

beta_first = 0.8
beta_second = 0.9
step_rate = 0.05
clip_level = 0.5
MESH = pl.DeviceIdType.MESH
F32 = jnp.float32
BF16 = jnp.bfloat16


def blend(grad, first, second):
    new_first = beta_first * first + (1.0 - beta_first) * grad
    new_second = beta_second * second + (1.0 - beta_second) * grad * grad
    return new_first, new_second


def exchange_kernel(
    nfs, nrep,
    xs0, xs1, ct0, ct1, fa0, fa1, m10, m20, m11, m21,
    low0, low1, grad0, grad1, tot_out,
    xin0, xin1, fb0, fb1, cv0, cv1, pb0, pb1, pt0, pt1, ra0, ra1, s0, s1, rb0, rb1,
    gb0, gb1, lb0, lb1, mo, tb, acc,
    lsem, xsem, zsem, bsem, csem, asem, rsem, gsem, lzsem, lxsem, tsem, osem,
):
    j = lax.axis_index("fs")
    r = lax.axis_index("rep")
    c = lax.axis_index("tp")
    mate = 1 - c
    xs, ct, fa, firsts, seconds = (xs0, xs1), (ct0, ct1), (fa0, fa1), (m10, m11), (m20, m21)
    lows, grads = (low0, low1), (grad0, grad1)
    xin, fb, cv, pb, pt, ra, sm, rb = (
        (xin0, xin1), (fb0, fb1), (cv0, cv1), (pb0, pb1), (pt0, pt1), (ra0, ra1), (s0, s1), (rb0, rb1),
    )
    gb, lb = (gb0, gb1), (lb0, lb1)
    rows = xs0.shape[0]
    depth, half = fb0.shape
    block = depth // nfs
    quarter = block // nrep
    chunk, width = rb0.shape[1:]
    zd = range(1, nfs)
    xd = range(1, nrep)

    def fs_at(d):
        return lax.rem(j + d + nfs, nfs)

    def rep_at(e):
        return lax.rem(r + e + nrep, nrep)

    def remote(src, dst, sems, idx, where):
        return pltpu.make_async_remote_copy(
            src_ref=src, dst_ref=dst, send_sem=sems.at[(0, *idx)], recv_sem=sems.at[(1, *idx)],
            device_id=where, device_id_type=MESH,
        )

    mine = pl.ds(pl.multiple_of(c * rows, rows), rows)
    half_cols = pl.ds(pl.multiple_of(c * half, half), half)
    own_rows = pl.ds(pl.multiple_of(j * block, block), block)
    mcols = pl.ds(pl.multiple_of(r * width, width), width)
    local = {}
    for f in (0, 1):
        local["x", f] = pltpu.make_async_copy(xs[f], xin[f].at[mine], lsem.at[0, f])
        local["f", f] = pltpu.make_async_copy(fa[f].at[:, half_cols], fb[f].at[own_rows], lsem.at[1, f])
        local["c", f] = pltpu.make_async_copy(ct[f], cv[f], lsem.at[2, f])
        local["1", f] = pltpu.make_async_copy(firsts[f].at[:, mcols], mo.at[f, 0], lsem.at[3, f])
        local["2", f] = pltpu.make_async_copy(seconds[f].at[:, mcols], mo.at[f, 1], lsem.at[4, f])

    barrier = pltpu.get_barrier_semaphore()
    for d in zd:
        pl.semaphore_signal(barrier, inc=1, device_id={"fs": fs_at(d)}, device_id_type=MESH)
    for e in xd:
        pl.semaphore_signal(barrier, inc=1, device_id={"rep": rep_at(e)}, device_id_type=MESH)
    pl.semaphore_signal(barrier, inc=1, device_id={"tp": mate}, device_id_type=MESH)
    for f in (0, 1):
        for k in ("x", "f", "c", "1", "2"):
            local[k, f].start()
    pl.semaphore_wait(barrier, nfs + nrep - 1)

    def frows(jj, rr):
        return pl.ds(pl.multiple_of(jj * block + rr * quarter, quarter), quarter)

    sends = []
    zcp = {}
    for f in (0, 1):
        for d in zd:
            cp = remote(
                fa[f].at[pl.ds(pl.multiple_of(r * quarter, quarter), quarter), half_cols],
                fb[f].at[frows(j, r)], zsem, (f, d - 1), {"fs": fs_at(d)},
            )
            cp.start()
            sends.append(cp)
            zcp[f, d] = remote(
                fa[f].at[pl.ds(pl.multiple_of(r * quarter, quarter), quarter), half_cols],
                fb[f].at[frows(fs_at(-d), r)], zsem, (f, d - 1), {"fs": fs_at(d)},
            )
    xcp = []
    for f in (0, 1):
        cp = remote(xs[f], xin[f].at[mine], xsem, (f,), {"tp": mate})
        cp.start()
        sends.append(cp)
        theirs = pl.ds(pl.multiple_of(mate * rows, rows), rows)
        xcp.append(remote(xs[f], xin[f].at[theirs], xsem, (f,), {"tp": mate}))
    for f in (0, 1):
        for d in zd:
            zcp[f, d].wait_recv()
            for e in xd:
                view = fb[f].at[frows(fs_at(-d), r)]
                cp = remote(view, view, bsem, (f, d - 1, e - 1), {"rep": rep_at(e)})
                cp.start()
                sends.append(cp)

    kstep = min(512, depth)
    perhalf = half // chunk

    for f in (0, 1):
        for k in ("x", "f", "c"):
            local[k, f].wait()
        xcp[f].wait_recv()
        for d in zd:
            for e in xd:
                view = fb[f].at[frows(fs_at(-d), rep_at(-e))]
                remote(view, view, bsem, (f, d - 1, e - 1), {"rep": rep_at(e)}).wait_recv()

        acc[...] = jnp.zeros_like(acc)

        def project(k, _, f=f):
            ks = pl.ds(pl.multiple_of(k * kstep, kstep), kstep)
            acc[...] += jnp.dot(xin[f][:, ks], fb[f][ks, :], preferred_element_type=F32)
            return 0

        lax.fori_loop(0, depth // kstep, project, 0)
        pb[f][c] = jnp.transpose(acc[...]).astype(BF16)
        cp = remote(pb[f].at[c], pb[f].at[c], csem, (f,), {"tp": mate})
        cp.start()
        sends.append(cp)

        def partials(h, f=f):
            left = pb[f][h]

            def piece(q, _):
                cols = pl.ds(pl.multiple_of(q * width, width), width)
                out = jnp.dot(left, cv[f][:, cols], preferred_element_type=F32)
                for i in range(perhalf):
                    pt[f][q, h * perhalf + i] = out[i * chunk:(i + 1) * chunk].astype(BF16)
                return 0

            lax.fori_loop(0, nrep, piece, 0)

        partials(c)
        remote(pb[f].at[mate], pb[f].at[mate], csem, (f,), {"tp": mate}).wait_recv()
        partials(mate)
        for e in xd:
            cp = remote(pt[f].at[rep_at(e)], ra[f].at[e - 1], asem, (f, e - 1), {"rep": rep_at(e)})
            cp.start()
            sends.append(cp)

    for f in (0, 1):
        for e in xd:
            remote(pt[f].at[rep_at(e)], ra[f].at[e - 1], asem, (f, e - 1), {"rep": rep_at(e)}).wait_recv()

        def add(i, _, f=f):
            total = pt[f][r, i].astype(F32)
            for e in xd:
                total += ra[f][e - 1, i].astype(F32)
            sm[f][i] = total.astype(BF16)
            return 0

        lax.fori_loop(0, nfs, add, 0)
        for d in zd:
            cp = remote(sm[f].at[fs_at(d)], rb[f].at[d - 1], rsem, (f, d - 1), {"fs": fs_at(d)})
            cp.start()
            sends.append(cp)

    for f in (0, 1):
        local["1", f].wait()
        local["2", f].wait()
        for d in zd:
            remote(sm[f].at[fs_at(d)], rb[f].at[d - 1], rsem, (f, d - 1), {"fs": fs_at(d)}).wait_recv()
        total = sm[f][j].astype(F32)
        for d in zd:
            total += rb[f][d - 1].astype(F32)
        kept = total.astype(BF16)
        gb[f][r] = kept
        new_first, new_second = blend(kept.astype(F32), mo[f, 0], mo[f, 1])
        lb[f][r, j] = (new_first / jnp.sqrt(new_second)).astype(BF16)
        for d in zd:
            view = lb[f].at[r, j]
            cp = remote(view, view, lzsem, (f, d - 1), {"fs": fs_at(d)})
            cp.start()
            sends.append(cp)
        for e in xd:
            view = lb[f].at[r, j]
            cp = remote(view, view, lxsem, (f, 0, e - 1), {"rep": rep_at(e)})
            cp.start()
            sends.append(cp)

    for f in (0, 1):
        for d in zd:
            view = lb[f].at[r, fs_at(-d)]
            remote(view, view, lzsem, (f, d - 1), {"fs": fs_at(d)}).wait_recv()
            for e in xd:
                cp = remote(view, view, lxsem, (f, d, e - 1), {"rep": rep_at(e)})
                cp.start()
                sends.append(cp)
    for f in (0, 1):
        for e in xd:
            cp = remote(gb[f].at[r], gb[f].at[r], gsem, (f, e - 1), {"rep": rep_at(e)})
            cp.start()
            sends.append(cp)
    for f in (0, 1):
        for d in range(nfs):
            for e in xd:
                view = lb[f].at[rep_at(-e), fs_at(-d)]
                remote(view, view, lxsem, (f, d, e - 1), {"rep": rep_at(e)}).wait_recv()
    outs = []
    for f in (0, 1):
        cp = pltpu.make_async_copy(lb[f], lows[f], osem.at[f, 0])
        cp.start()
        outs.append(cp)

    zero = jnp.zeros((chunk, width), F32)

    def square(i, carry):
        q, k = i // nfs, i % nfs
        for f in (0, 1):
            part = lb[f][q, k].astype(F32)
            carry = carry + part * part
        return carry

    squares = jnp.sum(lax.fori_loop(0, nrep * nfs, square, zero))
    tb[c] = jnp.full(tb.shape[1:], squares, F32)
    cp = remote(tb.at[c], tb.at[c], tsem, (), {"tp": mate})
    cp.start()
    sends.append(cp)
    for f in (0, 1):
        for e in xd:
            view = gb[f].at[rep_at(-e)]
            remote(view, view, gsem, (f, e - 1), {"rep": rep_at(e)}).wait_recv()
        cp = pltpu.make_async_copy(gb[f], grads[f], osem.at[f, 1])
        cp.start()
        outs.append(cp)
    remote(tb.at[mate], tb.at[mate], tsem, (), {"tp": mate}).wait_recv()
    tot_out[...] = tb[0] + tb[1]
    for cp in outs:
        cp.wait()
    for cp in sends:
        cp.wait_send()


def update_kernel(
    count, tot, low0, low1, grad0, grad1, fa0, fa1, w0, w1, m10, m20, m11, m21,
    nw0, cw0, nw1, cw1, n10, n20, n11, n21, st0, st1,
):
    spread = jnp.sqrt(tot[0:1, 0:1] / count)
    scale = clip_level / jnp.maximum(spread, clip_level)
    for grad, m1, m2, n1, n2, st in (
        (grad0, m10, m20, n10, n20, st0), (grad1, m11, m21, n11, n21, st1),
    ):
        new_first, new_second = blend(grad[0].astype(F32), m1[...], m2[...])
        n1[...] = new_first
        n2[...] = new_second
        low = (new_first / jnp.sqrt(new_second)).astype(BF16)
        st[...] = scale * low.astype(F32)
    full = jnp.dot(fa0[...], low0[0], preferred_element_type=F32)
    new = w0[...] - step_rate * scale * full
    nw0[...] = new
    cw0[...] = new.astype(BF16)
    full = lax.dot_general(low1[0], fa1[...], (((0,), (1,)), ((), ())), preferred_element_type=F32)
    new = w1[...] - step_rate * scale * full
    nw1[...] = new
    cw1[...] = new.astype(BF16)


def shards(nfs, nrep, ntp, xs0, xs1, ct0, ct1, fa0, fa1, w0, w1, m10, m20, m11, m21):
    rows, depth = xs0.shape
    tokens, chans = ct0.shape
    rank = fa0.shape[1]
    half = rank // ntp
    chunk = rank // nfs
    width = chans // nrep
    hbm = pl.BlockSpec(memory_space=pl.ANY)
    vmem = pl.BlockSpec(memory_space=pltpu.VMEM)
    sds = jax.ShapeDtypeStruct

    def twice(shape, dtype=BF16):
        return [pltpu.VMEM(shape, dtype)] * 2

    def sems(*shape):
        return pltpu.SemaphoreType.DMA(shape)

    low0, low1, grad0, grad1, tot = pl.pallas_call(
        functools.partial(exchange_kernel, nfs, nrep),
        out_shape=[sds((nrep, nfs, chunk, width), BF16)] * 2
        + [sds((nrep, chunk, width), BF16)] * 2
        + [sds((8, 128), F32)],
        in_specs=[hbm] * 10,
        out_specs=[hbm] * 4 + [vmem],
        scratch_shapes=twice((tokens, depth))
        + twice((depth, half))
        + twice((tokens, chans))
        + twice((ntp, half, tokens))
        + twice((nrep, nfs, chunk, width))
        + twice((nrep - 1, nfs, chunk, width))
        + twice((nfs, chunk, width))
        + twice((nfs - 1, chunk, width))
        + twice((nrep, chunk, width))
        + twice((nrep, nfs, chunk, width))
        + [pltpu.VMEM((2, 2, chunk, width), F32), pltpu.VMEM((ntp, 8, 128), F32), pltpu.VMEM((tokens, half), F32)]
        + [
            sems(5, 2),
            sems(2, 2),
            sems(2, 2, nfs - 1),
            sems(2, 2, nfs - 1, nrep - 1),
            sems(2, 2),
            sems(2, 2, nrep - 1),
            sems(2, 2, nfs - 1),
            sems(2, 2, nrep - 1),
            sems(2, 2, nfs - 1),
            sems(2, 2, nfs, nrep - 1),
            sems(2),
            sems(2, 2),
        ],
        compiler_params=pltpu.CompilerParams(
            collective_id=0, has_side_effects=True, vmem_limit_bytes=48 * 1024 * 1024
        ),
        name="exchange",
    )(xs0, xs1, ct0, ct1, fa0, fa1, m10, m20, m11, m21)
    low0 = low0.reshape(nrep, rank, width)
    low1 = low1.reshape(nrep, rank, width)

    block = fa0.shape[0]
    one = pl.BlockSpec((1, rank, width), lambda q: (q, 0, 0))
    gsp = pl.BlockSpec((1, chunk, width), lambda q: (q, 0, 0))
    whole = pl.BlockSpec((block, rank), lambda q: (0, 0))
    wcol = pl.BlockSpec((block, width), lambda q: (0, q))
    wrow = pl.BlockSpec((width, block), lambda q: (q, 0))
    msp = pl.BlockSpec((chunk, width), lambda q: (0, q))
    moment = sds((chunk, chans), F32)
    nw0, cw0, nw1, cw1, n10, n20, n11, n21, st0, st1 = pl.pallas_call(
        functools.partial(update_kernel, 2.0 * rank * chans * ntp),
        grid=(nrep,),
        out_shape=[
            sds((block, chans), F32), sds((block, chans), BF16),
            sds((chans, block), F32), sds((chans, block), BF16),
        ] + [moment] * 6,
        in_specs=[pl.BlockSpec((8, 128), lambda q: (0, 0)), one, one, gsp, gsp, whole, whole, wcol, wrow]
        + [msp] * 4,
        out_specs=[wcol, wcol, wrow, wrow] + [msp] * 6,
        compiler_params=pltpu.CompilerParams(vmem_limit_bytes=48 * 1024 * 1024),
        name="update",
    )(tot, low0, low1, grad0, grad1, fa0, fa1, w0, w1, m10, m20, m11, m21)
    return nw0, cw0, nw1, cw1, n10, n20, n11, n21, st0, st1


def solution(mesh):
    tokens = P(("fs", "rep", "tp"), None)
    mixed = P(("fs", "rep"), "tp")
    factor = P("fs", None)
    plain = P("fs", "tp")
    flipped = P("tp", "fs")
    sizes = mesh.shape
    return jax.shard_map(
        functools.partial(shards, sizes["fs"], sizes["rep"], sizes["tp"]),
        mesh=mesh,
        in_specs=(tokens, tokens, mixed, mixed, factor, factor, plain, flipped, plain, plain, plain, plain),
        out_specs=(plain, plain, flipped, flipped, plain, plain, plain, plain, plain, plain),
        check_vma=False,
    )
```

```python
import functools

import jax
import jax.numpy as jnp
from jax import lax
from jax.experimental import pallas as pl
from jax.experimental.pallas import tpu as pltpu
from jax.sharding import PartitionSpec as P

beta_first = 0.8
beta_second = 0.9
step_rate = 0.05
clip_level = 0.5
MESH = pl.DeviceIdType.MESH
F32 = jnp.float32
BF16 = jnp.bfloat16


def blend(grad, first, second):
    new_first = beta_first * first + (1.0 - beta_first) * grad
    new_second = beta_second * second + (1.0 - beta_second) * grad * grad
    return new_first, new_second


def exchange_kernel(
    nfs, nrep,
    xs0, xs1, ct0, ct1, fa0, fa1, m10, m20, m11, m21,
    low0, low1, grad0, grad1, tot_out,
    xin0, xin1, fb0, fb1, cv0, cv1, pb0, pb1, pt0, pt1, ra0, ra1, u0, u1, s0, s1, rb0, rb1,
    gb0, gb1, lb0, lb1, mo, tb, acc,
    lsem, xsem, zsem, bsem, csem, asem, rsem, gsem, lzsem, lxsem, tsem, osem,
):
    j = lax.axis_index("fs")
    r = lax.axis_index("rep")
    c = lax.axis_index("tp")
    mate = 1 - c
    xs, ct, fa, firsts, seconds = (xs0, xs1), (ct0, ct1), (fa0, fa1), (m10, m11), (m20, m21)
    lows, grads = (low0, low1), (grad0, grad1)
    xin, fb, cv, pb, pt, ra, sm, rb = (
        (xin0, xin1), (fb0, fb1), (cv0, cv1), (pb0, pb1), (pt0, pt1), (ra0, ra1), (s0, s1), (rb0, rb1),
    )
    gb, lb, ub = (gb0, gb1), (lb0, lb1), (u0, u1)
    rows = xs0.shape[0]
    depth, half = fb0.shape
    block = depth // nfs
    quarter = block // nrep
    chunk, width = rb0.shape[1:]
    zd = range(1, nfs)
    px = r + 1 - 2 * lax.rem(r, 2)
    py = lax.rem(r + 2, nrep)
    pd = nrep - 1 - r

    def fs_at(d):
        return lax.rem(j + d + nfs, nfs)

    def remote(src, dst, sems, idx, where):
        return pltpu.make_async_remote_copy(
            src_ref=src, dst_ref=dst, send_sem=sems.at[(0, *idx)], recv_sem=sems.at[(1, *idx)],
            device_id=where, device_id_type=MESH,
        )

    mine = pl.ds(pl.multiple_of(c * rows, rows), rows)
    half_cols = pl.ds(pl.multiple_of(c * half, half), half)
    own_rows = pl.ds(pl.multiple_of(j * block, block), block)
    local = {}
    for f in (0, 1):
        local["x", f] = pltpu.make_async_copy(xs[f], xin[f].at[mine], lsem.at[0, f])
        local["f", f] = pltpu.make_async_copy(fa[f].at[:, half_cols], fb[f].at[own_rows], lsem.at[1, f])
        local["c", f] = pltpu.make_async_copy(ct[f], cv[f], lsem.at[2, f])
        local["1", f] = pltpu.make_async_copy(firsts[f], mo.at[f, 0], lsem.at[3, f])
        local["2", f] = pltpu.make_async_copy(seconds[f], mo.at[f, 1], lsem.at[4, f])

    barrier = pltpu.get_barrier_semaphore()
    for d in zd:
        pl.semaphore_signal(barrier, inc=1, device_id={"fs": fs_at(d)}, device_id_type=MESH)
    for peer in (px, py):
        pl.semaphore_signal(barrier, inc=1, device_id={"rep": peer}, device_id_type=MESH)
    pl.semaphore_signal(barrier, inc=1, device_id={"tp": mate}, device_id_type=MESH)
    for f in (0, 1):
        for k in ("x", "f", "c", "1", "2"):
            local[k, f].start()
    pl.semaphore_wait(barrier, nfs - 1 + 2 + 1)

    def frows(jj, rr):
        return pl.ds(pl.multiple_of(jj * block + rr * quarter, quarter), quarter)

    sends = []

    def launch(cp):
        cp.start()
        sends.append(cp)

    class Spread:
        def __init__(self, view, sems, idx):
            self.view, self.sems, self.idx = view, sems, idx

        def copy(self, owner, part, k, peer):
            view = self.view(owner, part)
            return remote(view, view, self.sems, (*self.idx, k), {"rep": peer})

        def give(self):
            launch(self.copy(r, None, 0, px))
            launch(self.copy(r, None, 1, py))

        def relay(self):
            self.copy(px, None, 0, px).wait_recv()
            launch(self.copy(px, 0, 2, py))
            self.copy(py, None, 1, py).wait_recv()
            launch(self.copy(py, 1, 3, px))

        def finish(self):
            self.copy(pd, 0, 2, py).wait_recv()
            self.copy(pd, 1, 3, px).wait_recv()

    def lanes(size, part):
        return pl.ds(0, size) if part is None else pl.ds(part * (size // 2), size // 2)

    zcp = {}
    for f in (0, 1):
        for d in zd:
            cp = remote(
                fa[f].at[pl.ds(pl.multiple_of(r * quarter, quarter), quarter), half_cols],
                fb[f].at[frows(j, r)], zsem, (f, d - 1), {"fs": fs_at(d)},
            )
            cp.start()
            sends.append(cp)
            zcp[f, d] = remote(
                fa[f].at[pl.ds(pl.multiple_of(r * quarter, quarter), quarter), half_cols],
                fb[f].at[frows(fs_at(-d), r)], zsem, (f, d - 1), {"fs": fs_at(d)},
            )
    xcp = []
    for f in (0, 1):
        cp = remote(xs[f], xin[f].at[mine], xsem, (f,), {"tp": mate})
        cp.start()
        sends.append(cp)
        theirs = pl.ds(pl.multiple_of(mate * rows, rows), rows)
        xcp.append(remote(xs[f], xin[f].at[theirs], xsem, (f,), {"tp": mate}))
    fspread = {}
    last = None
    for f in (0, 1):
        for d in zd:
            zcp[f, d].wait_recv()
            item = Spread(
                lambda rr, part, f=f, d=d: fb[f].at[frows(fs_at(-d), rr), lanes(half, part)],
                bsem, (f, d - 1),
            )
            fspread[f, d] = item
            item.give()
            if last is not None:
                last.relay()
            last = item
    last.relay()

    def scatter(f, k):
        owner, peer = ((px, px), (pd, px), (py, py), (pd, py))[k]
        return remote(
            pt[f].at[owner, :, :, lanes(width, k // 2)], ra[f].at[k], asem, (f, k), {"rep": peer}
        )

    def second(f, part):
        return remote(ub[f].at[part], ra[f].at[4 + part], asem, (f, 4 + part), {"rep": (py, px)[part]})

    def lowered(f, q):
        cols = pl.ds(pl.multiple_of(q * width, width), width)
        new_first, new_second = blend(gb[f][q].astype(F32), mo[f, 0, :, cols], mo[f, 1, :, cols])
        lb[f][q, j] = (new_first / jnp.sqrt(new_second)).astype(BF16)

    kstep = min(512, depth)
    perhalf = half // chunk

    for f in (0, 1):
        for k in ("x", "f", "c"):
            local[k, f].wait()
        xcp[f].wait_recv()
        for d in zd:
            fspread[f, d].finish()

        acc[...] = jnp.zeros_like(acc)

        def project(k, _, f=f):
            ks = pl.ds(pl.multiple_of(k * kstep, kstep), kstep)
            acc[...] += jnp.dot(xin[f][:, ks], fb[f][ks, :], preferred_element_type=F32)
            return 0

        lax.fori_loop(0, depth // kstep, project, 0)
        pb[f][c] = jnp.transpose(acc[...]).astype(BF16)
        cp = remote(pb[f].at[c], pb[f].at[c], csem, (f,), {"tp": mate})
        cp.start()
        sends.append(cp)

        def partials(h, f=f):
            left = pb[f][h]

            def piece(q, _):
                cols = pl.ds(pl.multiple_of(q * width, width), width)
                out = jnp.dot(left, cv[f][:, cols], preferred_element_type=F32)
                for i in range(perhalf):
                    pt[f][q, h * perhalf + i] = out[i * chunk:(i + 1) * chunk].astype(BF16)
                return 0

            lax.fori_loop(0, nrep, piece, 0)

        partials(c)
        remote(pb[f].at[mate], pb[f].at[mate], csem, (f,), {"tp": mate}).wait_recv()
        partials(mate)
        for k in (1, 3, 0, 2):
            launch(scatter(f, k))

    for f in (0, 1):
        for k, owner, peer in ((1, py, py), (3, px, px)):
            scatter(f, k).wait_recv()
            part = k // 2
            cols = lanes(width, part)

            def fold(i, _, f=f, k=k, owner=owner, part=part, cols=cols):
                total = pt[f][owner, i, :, cols].astype(F32) + ra[f][k, i].astype(F32)
                ub[f][part, i] = total.astype(BF16)
                return 0

            lax.fori_loop(0, nfs, fold, 0)
            launch(second(f, part))
    for f in (0, 1):
        scatter(f, 0).wait_recv()
        scatter(f, 2).wait_recv()
        second(f, 0).wait_recv()
        second(f, 1).wait_recv()

        def add(i, _, f=f):
            for part in (0, 1):
                cols = lanes(width, part)
                total = pt[f][r, i, :, cols].astype(F32) + ra[f][2 * part, i].astype(F32)
                total += ra[f][4 + part, i].astype(F32)
                sm[f][i, :, cols] = total.astype(BF16)
            return 0

        lax.fori_loop(0, nfs, add, 0)
        for d in zd:
            cp = remote(sm[f].at[fs_at(d)], rb[f].at[d - 1], rsem, (f, d - 1), {"fs": fs_at(d)})
            cp.start()
            sends.append(cp)

    outs, gspread = [], []
    for f in (0, 1):
        local["1", f].wait()
        local["2", f].wait()
        for d in zd:
            remote(sm[f].at[fs_at(d)], rb[f].at[d - 1], rsem, (f, d - 1), {"fs": fs_at(d)}).wait_recv()
        total = sm[f][j].astype(F32)
        for d in zd:
            total += rb[f][d - 1].astype(F32)
        gb[f][r] = total.astype(BF16)
        lowered(f, r)
        for d in zd:
            view = lb[f].at[r, j]
            launch(remote(view, view, lzsem, (f, d - 1), {"fs": fs_at(d)}))
        gspread.append(Spread(lambda rr, part, f=f: gb[f].at[rr, :, lanes(width, part)], gsem, (f,)))
        gspread[f].give()
    for f in (0, 1):
        gspread[f].relay()

    lspread = []
    for f in (0, 1):
        for d in zd:
            view = lb[f].at[r, fs_at(-d)]
            remote(view, view, lzsem, (f, d - 1), {"fs": fs_at(d)}).wait_recv()
            item = Spread(
                lambda rr, part, f=f, d=d: lb[f].at[rr, fs_at(-d), :, lanes(width, part)],
                lxsem, (f, d - 1),
            )
            item.give()
            if lspread:
                lspread[-1].relay()
            lspread.append(item)
    lspread[-1].relay()
    for f in (0, 1):
        gspread[f].finish()
        cp = pltpu.make_async_copy(gb[f], grads[f], osem.at[f, 1])
        cp.start()
        outs.append(cp)
        for q in (px, py, pd):
            lowered(f, q)
    for item in lspread:
        item.finish()
    for f in (0, 1):
        cp = pltpu.make_async_copy(lb[f], lows[f], osem.at[f, 0])
        cp.start()
        outs.append(cp)

    zero = jnp.zeros((chunk, width), F32)

    def square(i, carry):
        q, k = i // nfs, i % nfs
        for f in (0, 1):
            part = lb[f][q, k].astype(F32)
            carry = carry + part * part
        return carry

    squares = jnp.sum(lax.fori_loop(0, nrep * nfs, square, zero))
    tb[c] = jnp.full(tb.shape[1:], squares, F32)
    cp = remote(tb.at[c], tb.at[c], tsem, (), {"tp": mate})
    cp.start()
    sends.append(cp)
    remote(tb.at[mate], tb.at[mate], tsem, (), {"tp": mate}).wait_recv()
    tot_out[...] = tb[0] + tb[1]
    for cp in outs:
        cp.wait()
    for cp in sends:
        cp.wait_send()


def update_kernel(
    count, tot, low0, low1, grad0, grad1, fa0, fa1, w0, w1, m10, m20, m11, m21,
    nw0, cw0, nw1, cw1, n10, n20, n11, n21, st0, st1,
):
    spread = jnp.sqrt(tot[0:1, 0:1] / count)
    scale = clip_level / jnp.maximum(spread, clip_level)
    for grad, m1, m2, n1, n2, st in (
        (grad0, m10, m20, n10, n20, st0), (grad1, m11, m21, n11, n21, st1),
    ):
        new_first, new_second = blend(grad[0].astype(F32), m1[...], m2[...])
        n1[...] = new_first
        n2[...] = new_second
        low = (new_first / jnp.sqrt(new_second)).astype(BF16)
        st[...] = scale * low.astype(F32)
    full = jnp.dot(fa0[...], low0[0], preferred_element_type=F32)
    new = w0[...] - step_rate * scale * full
    nw0[...] = new
    cw0[...] = new.astype(BF16)
    full = lax.dot_general(low1[0], fa1[...], (((0,), (1,)), ((), ())), preferred_element_type=F32)
    new = w1[...] - step_rate * scale * full
    nw1[...] = new
    cw1[...] = new.astype(BF16)


def shards(nfs, nrep, ntp, xs0, xs1, ct0, ct1, fa0, fa1, w0, w1, m10, m20, m11, m21):
    assert nrep == 4
    rows, depth = xs0.shape
    tokens, chans = ct0.shape
    rank = fa0.shape[1]
    half = rank // ntp
    chunk = rank // nfs
    width = chans // nrep
    hbm = pl.BlockSpec(memory_space=pltpu.HBM)
    free = pl.BlockSpec(memory_space=pl.ANY)
    vmem = pl.BlockSpec(memory_space=pltpu.VMEM)
    sds = jax.ShapeDtypeStruct

    def twice(shape, dtype=BF16):
        return [pltpu.VMEM(shape, dtype)] * 2

    def sems(*shape):
        return pltpu.SemaphoreType.DMA(shape)

    low0, low1, grad0, grad1, tot = pl.pallas_call(
        functools.partial(exchange_kernel, nfs, nrep),
        out_shape=[sds((nrep, nfs, chunk, width), BF16)] * 2
        + [sds((nrep, chunk, width), BF16)] * 2
        + [sds((8, 128), F32)],
        in_specs=[hbm] * 10,
        out_specs=[free] * 4 + [vmem],
        scratch_shapes=twice((tokens, depth))
        + twice((depth, half))
        + twice((tokens, chans))
        + twice((ntp, half, tokens))
        + twice((nrep, nfs, chunk, width))
        + twice((6, nfs, chunk, width // 2))
        + twice((2, nfs, chunk, width // 2))
        + twice((nfs, chunk, width))
        + twice((nfs - 1, chunk, width))
        + twice((nrep, chunk, width))
        + twice((nrep, nfs, chunk, width))
        + [pltpu.VMEM((2, 2, chunk, chans), F32), pltpu.VMEM((ntp, 8, 128), F32), pltpu.VMEM((tokens, half), F32)]
        + [
            sems(5, 2),
            sems(2, 2),
            sems(2, 2, nfs - 1),
            sems(2, 2, nfs - 1, 4),
            sems(2, 2),
            sems(2, 2, 6),
            sems(2, 2, nfs - 1),
            sems(2, 2, 4),
            sems(2, 2, nfs - 1),
            sems(2, 2, nfs - 1, 4),
            sems(2),
            sems(2, 2),
        ],
        compiler_params=pltpu.CompilerParams(
            collective_id=0, has_side_effects=True, vmem_limit_bytes=62 * 1024 * 1024
        ),
        name="exchange",
    )(xs0, xs1, ct0, ct1, fa0, fa1, m10, m20, m11, m21)
    low0 = low0.reshape(nrep, rank, width)
    low1 = low1.reshape(nrep, rank, width)

    block = fa0.shape[0]
    one = pl.BlockSpec((1, rank, width), lambda q: (q, 0, 0))
    gsp = pl.BlockSpec((1, chunk, width), lambda q: (q, 0, 0))
    whole = pl.BlockSpec((block, rank), lambda q: (0, 0))
    wcol = pl.BlockSpec((block, width), lambda q: (0, q))
    wrow = pl.BlockSpec((width, block), lambda q: (q, 0))
    msp = pl.BlockSpec((chunk, width), lambda q: (0, q))
    moment = sds((chunk, chans), F32)
    nw0, cw0, nw1, cw1, n10, n20, n11, n21, st0, st1 = pl.pallas_call(
        functools.partial(update_kernel, 2.0 * rank * chans * ntp),
        grid=(nrep,),
        out_shape=[
            sds((block, chans), F32), sds((block, chans), BF16),
            sds((chans, block), F32), sds((chans, block), BF16),
        ] + [moment] * 6,
        in_specs=[pl.BlockSpec((8, 128), lambda q: (0, 0)), one, one, gsp, gsp, whole, whole, wcol, wrow]
        + [msp] * 4,
        out_specs=[wcol, wcol, wrow, wrow] + [msp] * 6,
        compiler_params=pltpu.CompilerParams(vmem_limit_bytes=60 * 1024 * 1024),
        name="update",
    )(tot, low0, low1, grad0, grad1, fa0, fa1, w0, w1, m10, m20, m11, m21)
    return nw0, cw0, nw1, cw1, n10, n20, n11, n21, st0, st1


def solution(mesh):
    tokens = P(("fs", "rep", "tp"), None)
    mixed = P(("fs", "rep"), "tp")
    factor = P("fs", None)
    plain = P("fs", "tp")
    flipped = P("tp", "fs")
    sizes = mesh.shape
    return jax.shard_map(
        functools.partial(shards, sizes["fs"], sizes["rep"], sizes["tp"]),
        mesh=mesh,
        in_specs=(tokens, tokens, mixed, mixed, factor, factor, plain, flipped, plain, plain, plain, plain),
        out_specs=(plain, plain, flipped, flipped, plain, plain, plain, plain, plain, plain),
        check_vma=False,
    )
```

```python
import functools

import jax
import jax.numpy as jnp
from jax import lax
from jax.experimental import pallas as pl
from jax.experimental.pallas import tpu as pltpu
from jax.sharding import PartitionSpec as P

beta_first = 0.8
beta_second = 0.9
step_rate = 0.05
clip_level = 0.5
MESH = pl.DeviceIdType.MESH
F32 = jnp.float32
BF16 = jnp.bfloat16


def blend(grad, first, second):
    new_first = beta_first * first + (1.0 - beta_first) * grad
    new_second = beta_second * second + (1.0 - beta_second) * grad * grad
    return new_first, new_second


def exchange_kernel(
    nfs, nrep,
    xs0, xs1, ct0, ct1, fa0, fa1, m10, m20, m11, m21,
    low0, low1, grad0, grad1, tot_out,
    xin0, xin1, fb0, fb1, cv0, cv1, pb0, pb1, pt0, pt1, ra0, ra1, u0, u1, s0, s1, rb0, rb1,
    gb0, gb1, lb0, lb1, mo, tb, acc,
    lsem, xsem, zsem, bsem, csem, asem, rsem, gsem, lzsem, lxsem, tsem, osem,
):
    j = lax.axis_index("fs")
    r = lax.axis_index("rep")
    c = lax.axis_index("tp")
    mate = 1 - c
    xs, ct, fa, firsts, seconds = (xs0, xs1), (ct0, ct1), (fa0, fa1), (m10, m11), (m20, m21)
    lows, grads = (low0, low1), (grad0, grad1)
    xin, fb, cv, pb, pt, ra, sm, rb = (
        (xin0, xin1), (fb0, fb1), (cv0, cv1), (pb0, pb1), (pt0, pt1), (ra0, ra1), (s0, s1), (rb0, rb1),
    )
    gb, lb, ub = (gb0, gb1), (lb0, lb1), (u0, u1)
    rows = xs0.shape[0]
    depth, half = fb0.shape
    block = depth // nfs
    quarter = block // nrep
    chunk, width = rb0.shape[1:]
    zd = range(1, nfs)
    px = r + 1 - 2 * lax.rem(r, 2)
    py = lax.rem(r + 2, nrep)
    pd = nrep - 1 - r

    def fs_at(d):
        at = j
        for bit in (1 << i for i in range(d.bit_length())):
            if d & bit:
                at = at + bit - 2 * bit * lax.rem(lax.div(j, bit), 2)
        return at

    def remote(src, dst, sems, idx, where):
        return pltpu.make_async_remote_copy(
            src_ref=src, dst_ref=dst, send_sem=sems.at[(0, *idx)], recv_sem=sems.at[(1, *idx)],
            device_id=where, device_id_type=MESH,
        )

    mine = pl.ds(pl.multiple_of(c * rows, rows), rows)
    half_cols = pl.ds(pl.multiple_of(c * half, half), half)
    own_rows = pl.ds(pl.multiple_of(j * block, block), block)
    local = {}
    for f in (0, 1):
        local["x", f] = pltpu.make_async_copy(xs[f], xin[f].at[mine], lsem.at[0, f])
        local["f", f] = pltpu.make_async_copy(fa[f].at[:, half_cols], fb[f].at[own_rows], lsem.at[1, f])
        local["c", f] = pltpu.make_async_copy(ct[f], cv[f], lsem.at[2, f])
        local["1", f] = pltpu.make_async_copy(firsts[f], mo.at[f, 0], lsem.at[3, f])
        local["2", f] = pltpu.make_async_copy(seconds[f], mo.at[f, 1], lsem.at[4, f])

    barrier = pltpu.get_barrier_semaphore()
    for d in zd:
        pl.semaphore_signal(barrier, inc=1, device_id={"fs": fs_at(d)}, device_id_type=MESH)
    for peer in (px, py):
        pl.semaphore_signal(barrier, inc=1, device_id={"rep": peer}, device_id_type=MESH)
    pl.semaphore_signal(barrier, inc=1, device_id={"tp": mate}, device_id_type=MESH)
    for f in (0, 1):
        for k in ("x", "f", "c", "1", "2"):
            local[k, f].start()
    pl.semaphore_wait(barrier, nfs - 1 + 2 + 1)

    def frows(jj, rr):
        return pl.ds(pl.multiple_of(jj * block + rr * quarter, quarter), quarter)

    sends = []

    def launch(cp):
        cp.start()
        sends.append(cp)

    class Spread:
        def __init__(self, view, sems, idx):
            self.view, self.sems, self.idx = view, sems, idx

        def copy(self, owner, part, k, peer):
            view = self.view(owner, part)
            return remote(view, view, self.sems, (*self.idx, k), {"rep": peer})

        def give(self):
            launch(self.copy(r, None, 0, px))
            launch(self.copy(r, None, 1, py))

        def relay(self):
            self.copy(px, None, 0, px).wait_recv()
            launch(self.copy(px, 0, 2, py))
            self.copy(py, None, 1, py).wait_recv()
            launch(self.copy(py, 1, 3, px))

        def finish(self):
            self.copy(pd, 0, 2, py).wait_recv()
            self.copy(pd, 1, 3, px).wait_recv()

    def lanes(size, part):
        return pl.ds(0, size) if part is None else pl.ds(part * (size // 2), size // 2)

    zcp = {}
    for f in (0, 1):
        for d in zd:
            cp = remote(
                fa[f].at[pl.ds(pl.multiple_of(r * quarter, quarter), quarter), half_cols],
                fb[f].at[frows(j, r)], zsem, (f, d - 1), {"fs": fs_at(d)},
            )
            cp.start()
            sends.append(cp)
            zcp[f, d] = remote(
                fa[f].at[pl.ds(pl.multiple_of(r * quarter, quarter), quarter), half_cols],
                fb[f].at[frows(fs_at(d), r)], zsem, (f, d - 1), {"fs": fs_at(d)},
            )
    xcp = []
    for f in (0, 1):
        cp = remote(xs[f], xin[f].at[mine], xsem, (f,), {"tp": mate})
        cp.start()
        sends.append(cp)
        theirs = pl.ds(pl.multiple_of(mate * rows, rows), rows)
        xcp.append(remote(xs[f], xin[f].at[theirs], xsem, (f,), {"tp": mate}))
    def scatter(f, k):
        owner, peer = ((px, px), (pd, px), (py, py), (pd, py))[k]
        return remote(
            pt[f].at[owner, :, :, lanes(width, k // 2)], ra[f].at[k], asem, (f, k), {"rep": peer}
        )

    def second(f, part):
        return remote(ub[f].at[part], ra[f].at[4 + part], asem, (f, 4 + part), {"rep": (py, px)[part]})

    def halve(f):
        for k, owner in ((1, py), (3, px)):
            scatter(f, k).wait_recv()
            part = k // 2
            cols = lanes(width, part)

            def fold(i, _, k=k, owner=owner, part=part, cols=cols):
                total = pt[f][owner, i, :, cols].astype(F32) + ra[f][k, i].astype(F32)
                ub[f][part, i] = total.astype(BF16)
                return 0

            lax.fori_loop(0, nfs, fold, 0)
            launch(second(f, part))

    def lowered(f, q):
        cols = pl.ds(pl.multiple_of(q * width, width), width)
        new_first, new_second = blend(gb[f][q].astype(F32), mo[f, 0, :, cols], mo[f, 1, :, cols])
        lb[f][q, j] = (new_first / jnp.sqrt(new_second)).astype(BF16)

    kstep = min(512, depth)
    perhalf = half // chunk

    fspread = {}

    def compute(f):
        for k in ("x", "f", "c"):
            local[k, f].wait()
        xcp[f].wait_recv()
        for d in zd:
            fspread[f, d].finish()

        acc[...] = jnp.zeros_like(acc)

        def project(k, _, f=f):
            ks = pl.ds(pl.multiple_of(k * kstep, kstep), kstep)
            acc[...] += jnp.dot(xin[f][:, ks], fb[f][ks, :], preferred_element_type=F32)
            return 0

        lax.fori_loop(0, depth // kstep, project, 0)
        pb[f][c] = jnp.transpose(acc[...]).astype(BF16)
        cp = remote(pb[f].at[c], pb[f].at[c], csem, (f,), {"tp": mate})
        cp.start()
        sends.append(cp)

        def partials(h, f=f):
            left = pb[f][h]

            def piece(q, _):
                cols = pl.ds(pl.multiple_of(q * width, width), width)
                out = jnp.dot(left, cv[f][:, cols], preferred_element_type=F32)
                for i in range(perhalf):
                    pt[f][q, h * perhalf + i] = out[i * chunk:(i + 1) * chunk].astype(BF16)
                return 0

            lax.fori_loop(0, nrep, piece, 0)

        partials(c)
        remote(pb[f].at[mate], pb[f].at[mate], csem, (f,), {"tp": mate}).wait_recv()
        partials(mate)
    last = None
    for f in (0, 1):
        for d in zd:
            zcp[f, d].wait_recv()
            item = Spread(
                lambda rr, part, f=f, d=d: fb[f].at[frows(fs_at(d), rr), lanes(half, part)],
                bsem, (f, d - 1),
            )
            fspread[f, d] = item
            item.give()
            if last is not None:
                last.relay()
            last = item
    compute(0)
    last.relay()
    for k in (1, 3, 0, 2):
        launch(scatter(0, k))
    compute(1)
    for k in (1, 3):
        launch(scatter(1, k))
    halve(0)
    for k in (0, 2):
        launch(scatter(1, k))
    halve(1)

    for f in (0, 1):
        scatter(f, 0).wait_recv()
        scatter(f, 2).wait_recv()
        second(f, 0).wait_recv()
        second(f, 1).wait_recv()

        def add(i, _, f=f):
            for part in (0, 1):
                cols = lanes(width, part)
                total = pt[f][r, i, :, cols].astype(F32) + ra[f][2 * part, i].astype(F32)
                total += ra[f][4 + part, i].astype(F32)
                sm[f][i, :, cols] = total.astype(BF16)
            return 0

        lax.fori_loop(0, nfs, add, 0)
        for d in zd:
            cp = remote(sm[f].at[fs_at(d)], rb[f].at[d - 1], rsem, (f, d - 1), {"fs": fs_at(d)})
            cp.start()
            sends.append(cp)

    outs, gspread = [], []
    for f in (0, 1):
        local["1", f].wait()
        local["2", f].wait()
        for d in zd:
            remote(sm[f].at[fs_at(d)], rb[f].at[d - 1], rsem, (f, d - 1), {"fs": fs_at(d)}).wait_recv()
        total = sm[f][j].astype(F32)
        for d in zd:
            total += rb[f][d - 1].astype(F32)
        gb[f][r] = total.astype(BF16)
        lowered(f, r)
        for d in zd:
            view = lb[f].at[r, j]
            launch(remote(view, view, lzsem, (f, d - 1), {"fs": fs_at(d)}))
        gspread.append(Spread(lambda rr, part, f=f: gb[f].at[rr, :, lanes(width, part)], gsem, (f,)))
        gspread[f].give()
    for f in (0, 1):
        gspread[f].relay()

    lspread = []
    for f in (0, 1):
        for d in zd:
            view = lb[f].at[r, fs_at(d)]
            remote(view, view, lzsem, (f, d - 1), {"fs": fs_at(d)}).wait_recv()
            item = Spread(
                lambda rr, part, f=f, d=d: lb[f].at[rr, fs_at(d), :, lanes(width, part)],
                lxsem, (f, d - 1),
            )
            item.give()
            if lspread:
                lspread[-1].relay()
            lspread.append(item)
    lspread[-1].relay()
    for f in (0, 1):
        gspread[f].finish()
        cp = pltpu.make_async_copy(gb[f], grads[f], osem.at[f, 1])
        cp.start()
        outs.append(cp)
        for q in (px, py, pd):
            lowered(f, q)
    for item in lspread:
        item.finish()
    for f in (0, 1):
        cp = pltpu.make_async_copy(lb[f], lows[f], osem.at[f, 0])
        cp.start()
        outs.append(cp)

    zero = jnp.zeros((chunk, width), F32)

    def square(i, carry):
        q, k = i // nfs, i % nfs
        for f in (0, 1):
            part = lb[f][q, k].astype(F32)
            carry = carry + part * part
        return carry

    squares = jnp.sum(lax.fori_loop(0, nrep * nfs, square, zero))
    tb[c] = jnp.full(tb.shape[1:], squares, F32)
    cp = remote(tb.at[c], tb.at[c], tsem, (), {"tp": mate})
    cp.start()
    sends.append(cp)
    remote(tb.at[mate], tb.at[mate], tsem, (), {"tp": mate}).wait_recv()
    tot_out[...] = tb[0] + tb[1]
    for cp in outs:
        cp.wait()
    for cp in sends:
        cp.wait_send()


def update_kernel(
    count, tot, low0, low1, grad0, grad1, fa0, fa1, w0, w1, m10, m20, m11, m21,
    nw0, cw0, nw1, cw1, n10, n20, n11, n21, st0, st1,
):
    spread = jnp.sqrt(tot[0:1, 0:1] / count)
    scale = clip_level / jnp.maximum(spread, clip_level)
    for grad, m1, m2, n1, n2, st in (
        (grad0, m10, m20, n10, n20, st0), (grad1, m11, m21, n11, n21, st1),
    ):
        new_first, new_second = blend(grad[0].astype(F32), m1[...], m2[...])
        n1[...] = new_first
        n2[...] = new_second
        low = (new_first / jnp.sqrt(new_second)).astype(BF16)
        st[...] = scale * low.astype(F32)
    full = jnp.dot(fa0[...], low0[0], preferred_element_type=F32)
    new = w0[...] - step_rate * scale * full
    nw0[...] = new
    cw0[...] = new.astype(BF16)
    full = lax.dot_general(low1[0], fa1[...], (((0,), (1,)), ((), ())), preferred_element_type=F32)
    new = w1[...] - step_rate * scale * full
    nw1[...] = new
    cw1[...] = new.astype(BF16)


def shards(nfs, nrep, ntp, xs0, xs1, ct0, ct1, fa0, fa1, w0, w1, m10, m20, m11, m21):
    assert nrep == 4 and nfs & (nfs - 1) == 0
    rows, depth = xs0.shape
    tokens, chans = ct0.shape
    rank = fa0.shape[1]
    half = rank // ntp
    chunk = rank // nfs
    width = chans // nrep
    hbm = pl.BlockSpec(memory_space=pltpu.HBM)
    free = pl.BlockSpec(memory_space=pl.ANY)
    vmem = pl.BlockSpec(memory_space=pltpu.VMEM)
    sds = jax.ShapeDtypeStruct

    def twice(shape, dtype=BF16):
        return [pltpu.VMEM(shape, dtype)] * 2

    def sems(*shape):
        return pltpu.SemaphoreType.DMA(shape)

    low0, low1, grad0, grad1, tot = pl.pallas_call(
        functools.partial(exchange_kernel, nfs, nrep),
        out_shape=[sds((nrep, nfs, chunk, width), BF16)] * 2
        + [sds((nrep, chunk, width), BF16)] * 2
        + [sds((8, 128), F32)],
        in_specs=[hbm] * 10,
        out_specs=[free] * 4 + [vmem],
        scratch_shapes=twice((tokens, depth))
        + twice((depth, half))
        + twice((tokens, chans))
        + twice((ntp, half, tokens))
        + twice((nrep, nfs, chunk, width))
        + twice((6, nfs, chunk, width // 2))
        + twice((2, nfs, chunk, width // 2))
        + twice((nfs, chunk, width))
        + twice((nfs - 1, chunk, width))
        + twice((nrep, chunk, width))
        + twice((nrep, nfs, chunk, width))
        + [pltpu.VMEM((2, 2, chunk, chans), F32), pltpu.VMEM((ntp, 8, 128), F32), pltpu.VMEM((tokens, half), F32)]
        + [
            sems(5, 2),
            sems(2, 2),
            sems(2, 2, nfs - 1),
            sems(2, 2, nfs - 1, 4),
            sems(2, 2),
            sems(2, 2, 6),
            sems(2, 2, nfs - 1),
            sems(2, 2, 4),
            sems(2, 2, nfs - 1),
            sems(2, 2, nfs - 1, 4),
            sems(2),
            sems(2, 2),
        ],
        compiler_params=pltpu.CompilerParams(
            collective_id=0, has_side_effects=True, vmem_limit_bytes=62 * 1024 * 1024
        ),
        name="exchange",
    )(xs0, xs1, ct0, ct1, fa0, fa1, m10, m20, m11, m21)
    low0 = low0.reshape(nrep, rank, width)
    low1 = low1.reshape(nrep, rank, width)

    block = fa0.shape[0]
    one = pl.BlockSpec((1, rank, width), lambda q: (q, 0, 0))
    gsp = pl.BlockSpec((1, chunk, width), lambda q: (q, 0, 0))
    whole = pl.BlockSpec((block, rank), lambda q: (0, 0))
    wcol = pl.BlockSpec((block, width), lambda q: (0, q))
    wrow = pl.BlockSpec((width, block), lambda q: (q, 0))
    msp = pl.BlockSpec((chunk, width), lambda q: (0, q))
    moment = sds((chunk, chans), F32)
    nw0, cw0, nw1, cw1, n10, n20, n11, n21, st0, st1 = pl.pallas_call(
        functools.partial(update_kernel, 2.0 * rank * chans * ntp),
        grid=(nrep,),
        out_shape=[
            sds((block, chans), F32), sds((block, chans), BF16),
            sds((chans, block), F32), sds((chans, block), BF16),
        ] + [moment] * 6,
        in_specs=[pl.BlockSpec((8, 128), lambda q: (0, 0)), one, one, gsp, gsp, whole, whole, wcol, wrow]
        + [msp] * 4,
        out_specs=[wcol, wcol, wrow, wrow] + [msp] * 6,
        compiler_params=pltpu.CompilerParams(vmem_limit_bytes=60 * 1024 * 1024),
        name="update",
    )(tot, low0, low1, grad0, grad1, fa0, fa1, w0, w1, m10, m20, m11, m21)
    return nw0, cw0, nw1, cw1, n10, n20, n11, n21, st0, st1


def solution(mesh):
    tokens = P(("fs", "rep", "tp"), None)
    mixed = P(("fs", "rep"), "tp")
    factor = P("fs", None)
    plain = P("fs", "tp")
    flipped = P("tp", "fs")
    sizes = mesh.shape
    return jax.shard_map(
        functools.partial(shards, sizes["fs"], sizes["rep"], sizes["tp"]),
        mesh=mesh,
        in_specs=(tokens, tokens, mixed, mixed, factor, factor, plain, flipped, plain, plain, plain, plain),
        out_specs=(plain, plain, flipped, flipped, plain, plain, plain, plain, plain, plain),
        check_vma=False,
    )
```
